1024 devices in a mesh: fs: 64 (over z, core), tp: 16 (over y, x).
Axes of the slice: x: 4, y: 4, z: 32, core: 2. Of those that a mesh axis runs over, the one named last changes fastest.
Arguments:
- prompt: bfloat16 [4096, 2048], P('tp'), may hold values from -6 to 6
- norm_gain: float32 [2048], P('fs'), may hold values from 0.1 to 1.9
- gate_master: float32 [32, 2048, 512], P(None, 'fs', 'tp'), may hold values from -6 to 6
- up_master: float32 [32, 2048, 512], P(None, 'fs', 'tp'), may hold values from -6 to 6
- down_master: float32 [32, 2048, 512], P(None, 'fs', 'tp'), may hold values from -6 to 6
- group_choice: int32 [4096], P('tp'), may hold values from 0 to 3
- inner_choice: int32 [4096, 2], P('tp'), may hold values from 0 to 7, as said below
- route_weight: float32 [4096, 2], P('tp'), may hold values from 0.2 to 1
Outputs:
- gate_served: bfloat16 [2048, 16384], P(None, 'fs')
- up_served: bfloat16 [2048, 16384], P(None, 'fs')
- down_served: bfloat16 [2048, 16384], P(None, 'fs')
- mixed: bfloat16 [4096, 2048], P('tp', 'fs')
The draws below stay inside these ranges and needn't reach their ends.
Inputs may be any that keep to these rules, and one draw needn't show every extreme that they name: `inner_choice`: the two experts of a token differ.
All inputs are finite; a program needn't handle non-finite values.
Results may differ from the reference program's by a relative error of at most 0.0081.
Values may be sent and summed in bfloat16 or wider, within the bound.
A program may use at most 64 MiB of HBM per device.

```python
import math
import jax
import jax.numpy as jnp
from jax import lax

D = 2048
FF = 512
GROUPS = 4
EPG = 8
TOK_DEV = 256
EXPERTS = 32
TOKENS = 4096


def routing_draw(key):
    base = jax.random.fold_in(key, 7411)
    keys = jax.random.split(base, 9)
    shards = TOKENS // TOK_DEV
    hot_group = jax.random.randint(keys[0], (shards,), 0, GROUPS)
    hot_inner = jax.random.randint(keys[1], (shards,), 0, EPG)
    hot_count = jax.random.randint(keys[2], (shards,), 0, TOK_DEV // 2 + 1)
    heavy = jax.random.randint(keys[3], (), 0, shards)
    hot_count = jnp.where(jnp.arange(shards) == heavy, 3 * TOK_DEV // 4, hot_count)
    ranks = jax.vmap(lambda sub: jax.random.permutation(sub, TOK_DEV))(jax.random.split(keys[4], shards))
    hot = (ranks < hot_count[:, None]).reshape(TOKENS)
    shard_of = jnp.arange(TOKENS) // TOK_DEV
    drawn_group = jax.random.randint(keys[5], (TOKENS,), 0, GROUPS)
    first_drawn = jax.random.randint(keys[6], (TOKENS,), 0, EPG)
    offsets = jax.random.randint(keys[7], (TOKENS,), 1, EPG)
    flip = jax.random.randint(keys[8], (TOKENS,), 0, 2)
    group = jnp.where(hot, hot_group[shard_of], drawn_group)
    first = jnp.where(hot, hot_inner[shard_of], first_drawn)
    second = (first + offsets) % EPG
    pair = jnp.where(flip[:, None] == 1, jnp.stack([second, first], axis=1), jnp.stack([first, second], axis=1))
    return (group.astype(jnp.int32), pair.astype(jnp.int32))


def draw_group_choice(key, part):
    group, pair = routing_draw(key)
    return group


def draw_inner_choice(key, part):
    group, pair = routing_draw(key)
    return pair


def levels(key, shape, cuts, smallest, high):
    def one(dim, blocks):
        steps = jax.random.uniform(jax.random.fold_in(jax.random.fold_in(key, 6), dim), (blocks,), jnp.float32, smallest / len(cuts), high / len(cuts))
        return jnp.repeat(jnp.exp(steps), shape[dim] // blocks).reshape((-1,) + (1,) * (len(shape) - dim - 1))

    loudness = one(*cuts[0])
    for cut in cuts[1:]:
        loudness = loudness * one(*cut)
    return loudness


def scatter_about(rng, extent, scale, reach, pieces=(), kind=jnp.bfloat16):
    drawn = jax.random.normal(rng, extent, jnp.float32) * scale
    if len(pieces) > 0:
        drawn = levels(rng, extent, pieces, -0.22, 0.18) * drawn
    return jnp.clip(drawn, min=-reach, max=reach).astype(kind)


def setup_inputs(seed: int = 0) -> dict:
    seeds = jax.random.split(jax.random.key(seed), 9)
    prompt = scatter_about(seeds[0], (TOKENS, D), 1.0, 6.0, ((0, 16),))
    norm_gain = jnp.clip(1.0 + 0.18 * jax.random.normal(seeds[1], (D,), jnp.float32), 0.1, 1.9)
    gate_master = scatter_about(seeds[2], (EXPERTS, D, FF), 1.0, 6.0, ((1, 64), (2, 16)), jnp.float32)
    up_master = scatter_about(seeds[3], (EXPERTS, D, FF), 1.0, 6.0, ((1, 64), (2, 16)), jnp.float32)
    down_master = scatter_about(seeds[4], (EXPERTS, D, FF), 1.0, 6.0, ((1, 64), (2, 16)), jnp.float32)
    group_choice = draw_group_choice(jax.random.fold_in(seeds[8], 71), 0)
    inner_choice = draw_inner_choice(jax.random.fold_in(seeds[8], 71), 0)
    route_weight = jnp.clip(jnp.exp(math.log(1.0) - 1.609438 * jax.random.uniform(seeds[7], (TOKENS, 2), jnp.float32) ** levels(seeds[7], (TOKENS, 2), ((0, 16),), -0.2, 0.2)), 0.2, 1.0)
    return dict(prompt=prompt, norm_gain=norm_gain, gate_master=gate_master, up_master=up_master, down_master=down_master, group_choice=group_choice, inner_choice=inner_choice, route_weight=route_weight)


def reference(prompt, norm_gain, gate_master, up_master, down_master, group_choice, inner_choice, route_weight):
    experts = GROUPS * EPG
    scale = norm_gain[None, :, None]
    gate_served = (gate_master * scale).astype(jnp.bfloat16).transpose(1, 0, 2).reshape(D, experts * FF)
    up_served = (up_master * scale).astype(jnp.bfloat16).transpose(1, 0, 2).reshape(D, experts * FF)
    down_served = down_master.astype(jnp.bfloat16).transpose(1, 0, 2).reshape(D, experts * FF)
    values = prompt.astype(jnp.float32)
    normed = (values * lax.rsqrt(lax.optimization_barrier(jnp.mean(values * values, axis=1, keepdims=True)) + 1e-06)).astype(jnp.bfloat16)
    chosen = group_choice[:, None] * EPG + inner_choice
    member = (chosen[:, :, None] == jnp.arange(experts, dtype=jnp.int32)[None, None, :]).astype(jnp.float32)
    weight = lax.optimization_barrier(jnp.sum(member * route_weight[:, :, None], axis=1))

    def one_expert(total, index):
        begin = (index * FF).astype(jnp.int32)
        gate_cols = lax.dynamic_slice_in_dim(gate_served, begin, FF, 1)
        up_cols = lax.dynamic_slice_in_dim(up_served, begin, FF, 1)
        down_cols = lax.dynamic_slice_in_dim(down_served, begin, FF, 1)
        gate_act = jnp.dot(normed, gate_cols, preferred_element_type=jnp.float32) * D ** (-0.5)
        up_act = jnp.dot(normed, up_cols, preferred_element_type=jnp.float32) * D ** (-0.5)
        column = lax.dynamic_slice_in_dim(weight, index.astype(jnp.int32), 1, 1)
        scaled = (column * jax.nn.silu(gate_act) * up_act).astype(jnp.bfloat16)
        part = lax.dot_general(scaled, down_cols, (((1,), (1,)), ((), ())), preferred_element_type=jnp.float32)
        return (total + part, None)
    total, _ = lax.scan(one_expert, jnp.zeros((prompt.shape[0], D), jnp.float32), jnp.arange(experts, dtype=jnp.int32))
    mixed = (total * FF ** (-0.5)).astype(jnp.bfloat16)
    return (gate_served, up_served, down_served, mixed)
```

```python
import jax
import jax.numpy as jnp
import numpy as np
from jax import lax
from jax.experimental import pallas as pl
from jax.experimental.pallas import tpu as pltpu
from jax.sharding import PartitionSpec as P

FF = 512
EPG = 8
MESH = pl.DeviceIdType.MESH
BVAL = (0, 1, -1, 2)
WAVE_AT = (0, 8, 24, 40, 56)
WAVE_N = (8, 16, 16, 16, 8)


def place():
    fs = lax.axis_index("fs")
    tp = lax.axis_index("tp")
    return fs // 2, fs % 2, tp // 4, tp % 4


def device(z, c, y, x):
    return {"fs": lax.rem(z + 32, 32) * 2 + c, "tp": lax.rem(y + 4, 4) * 4 + lax.rem(x + 4, 4)}


class Copies:
    def __init__(self, send, recv):
        self.send, self.recv, self.used, self.pending = send, recv, 0, []

    def slots(self, n=1):
        at = self.used
        self.used += n
        return at

    def make(self, src, dst, dev, at, to=0):
        return pltpu.make_async_remote_copy(
            src_ref=src,
            dst_ref=dst,
            send_sem=self.send.at[at],
            recv_sem=self.recv.at[at + to],
            device_id=dev,
            device_id_type=MESH,
        )

    def start(self, src, dst, dev, at, to=0, when=None):
        def go():
            self.make(src, dst, dev, at, to).start()

        def end():
            self.make(src, dst, dev, at, to).wait_send()

        if when is None:
            go()
        else:
            pl.when(when)(go)
        self.pending.append((when, end))

    def arrived(self, ref, dev, at, to=0):
        self.make(ref, ref, dev, at, to).wait_recv()

    def drain(self):
        for when, end in self.pending:
            if when is None:
                end()
            else:
                pl.when(when)(end)


def greet(partners, meanwhile=None):
    barrier = pltpu.get_barrier_semaphore()
    for dev in partners:
        pl.semaphore_signal(barrier, inc=1, device_id=dev, device_id_type=MESH)
    if meanwhile is not None:
        meanwhile()
    pl.semaphore_wait(barrier, len(partners))


def pack(gain_ref, held, s_ref, loads):
    for load in loads:
        load.start()
    eye = lax.broadcasted_iota(jnp.int32, (32, 32), 0) == lax.broadcasted_iota(jnp.int32, (32, 32), 1)
    gain = jnp.sum(jnp.where(eye, gain_ref[...], 0.0), axis=1, keepdims=True)
    hidden = lax.broadcasted_iota(jnp.int32, (32, 128), 0)
    lane = lax.broadcasted_iota(jnp.int32, (32, 128), 1)
    for n, load in enumerate(loads):
        load.wait()
        total = jnp.zeros((256, 128), jnp.float32)
        for q in range(4):
            rows = held[n, :, 8 * q : 8 * q + 8, :]
            if n < 2:
                rows = rows * gain[8 * q : 8 * q + 8][None]
            place_q = (lane == hidden + 32 * q).astype(jnp.float32).astype(jnp.bfloat16)
            total += jnp.dot(
                rows.reshape(256, 32).astype(jnp.bfloat16), place_q, preferred_element_type=jnp.float32
            )
        for e in range(32):
            s_ref[e % 4, e // 4, 8 * n : 8 * n + 8] = total[8 * e : 8 * e + 8].astype(jnp.bfloat16)


def move_kernel(
    gate_ref, up_ref, down_ref, gain_ref, f_out, held, f_ref, s_ref, abuf, bbuf, load, store, send, recv
):
    z, c, y, x = place()
    s = 1 - 2 * c
    k = z // 4
    owner = y // 2
    jy = y % 2
    rel = lax.rem(y - 2 * c + 4, 4)
    owns = rel < 2
    other = device(z, 1 - c, y, x)
    right, left = device(z, c, y, x + 1), device(z, c, y, x - 1)
    up, down = device(z, c, y + 1, x), device(z, c, y - 1, x)
    greet(
        [device(z + d, c, y, x) for d in (1, -1, 2, -2, 4, -4)]
        + [device(z + d, 1 - c, y, x) for d in (4, -4)]
        + [other, right, left, up, down],
        lambda: pack(
            gain_ref,
            held,
            s_ref,
            [
                pltpu.make_async_copy(m, held.at[n], load.at[n])
                for n, m in enumerate((gate_ref, up_ref, down_ref))
            ],
        ),
    )
    cp = Copies(send, recv)

    a_at = cp.slots(3)
    for i in (3, 1, 2):
        b = BVAL[i] * s
        cp.start(s_ref.at[lax.rem(z + b + 32, 4)], abuf.at[i], device(z + b, c, y, x), a_at + i - 1)
    abuf[0] = s_ref[lax.rem(z, 4)]
    for i in (1, 2, 3):
        cp.arrived(abuf.at[i], other, a_at + i - 1)

    def slot(a, direction):
        w = abs(a)
        if w in (0, 4):
            return WAVE_AT[w] + c * 4
        return WAVE_AT[w] + (0 if direction > 0 else 8) + c * 4

    hop = {}
    final = {}

    def stride_step(n, a):
        for side, direction in ((0, 1), (1, -1)):
            via = device(z + 4 * direction, c, y, x)
            end = device(z + 4 * direction, owner, y, x)
            half = pl.ds(2 * side, 2) if a == 4 else pl.ds(0, 4)
            width = 2 if a == 4 else 4
            if n == 1:
                src = abuf.at[half, lax.rem(k + direction * a + 8, 8)]
            else:
                src = bbuf.at[side, n - 2, a - 2, pl.ds(0, width)]
                cp.arrived(src, other, hop[side, n - 1, a])
            if a == n:
                at = cp.slots(2)
                first = slot(a, direction) + (2 * side if a == 4 else 0)
                cp.start(src, f_ref.at[jy, x, pl.ds(first, width)], end, at, c)
                final[side, a] = (at, width)
            else:
                at = cp.slots(1)
                hop[side, n, a] = at
                cp.start(src, bbuf.at[side, n - 1, a - 2, pl.ds(0, width)], via, at)

    zero_at = cp.slots(1)

    def wave_arrived(w):
        if w == 0:

            @pl.when(owns)
            def _():
                f_ref[jy, x, pl.ds(c * 4, 4)] = abuf[:, k]
                cp.arrived(f_ref.at[jy, x, pl.ds((1 - c) * 4, 4)], other, zero_at)

            return

        @pl.when(owns)
        def _():
            for side in (0, 1):
                at, width = final[side, w]
                for core in (0, 1):
                    cp.arrived(f_ref.at[jy, x, pl.ds(0, width)], other, at, core)

    ring = {}

    def ring_x(key, take, when):
        def first():
            at = ring[key] = cp.slots(4)
            cp.start(take(x, 0), take(x, 0), right, at, when=when)
            cp.start(take(x, 0), take(x, 0), left, at + 1, when=when)

        def second():
            at = ring[key]

            def wait():
                cp.arrived(take(lax.rem(x + 3, 4), 0), other, at)
                cp.arrived(take(lax.rem(x + 1, 4), 0), other, at + 1)

            if when is None:
                wait()
            else:
                pl.when(when)(wait)
            cp.start(take(lax.rem(x + 3, 4), 1), take(lax.rem(x + 3, 4), 1), right, at + 2, when=when)
            cp.start(take(lax.rem(x + 1, 4), 2), take(lax.rem(x + 1, 4), 2), left, at + 3, when=when)

        def last():
            at = ring[key]

            def wait():
                cp.arrived(take(lax.rem(x + 2, 4), 1), other, at + 2)
                cp.arrived(take(lax.rem(x + 2, 4), 2), other, at + 3)

            if when is None:
                wait()
            else:
                pl.when(when)(wait)

        return first, second, last

    plus = (rel == 1) | (rel == 2)
    minus = (rel == 0) | (rel == 3)
    got = 1 - lax.rem(rel, 2)

    def ring_y(key, take):
        def first():
            at = ring[key] = cp.slots(4)
            cp.start(take(jy, 0), take(jy, 0), up, at, when=owns)
            cp.start(take(jy, 0), take(jy, 0), down, at + 1, when=owns)

        def second():
            at = ring[key]

            @pl.when(plus)
            def _():
                cp.arrived(take(got, 0), other, at)

            @pl.when(minus)
            def _():
                cp.arrived(take(got, 0), other, at + 1)

            cp.start(take(got, 1), take(got, 1), up, at + 2, when=plus)
            cp.start(take(got, 2), take(got, 2), down, at + 3, when=minus)

        def last():
            at = ring[key]

            @pl.when(jnp.logical_not(owns))
            def _():
                cp.arrived(take(jy, 1), other, at + 2)
                cp.arrived(take(jy, 2), other, at + 3)

        return first, second, last

    def out(w):
        slots = pl.ds(WAVE_AT[w], WAVE_N[w])
        return pltpu.make_async_copy(f_ref.at[:, :, slots], f_out.at[:, :, slots], store.at[w])

    def wave(w):
        n = WAVE_N[w] // 2
        h1, h2 = WAVE_AT[w], WAVE_AT[w] + n

        def part(base, p):
            return pl.ds(base, n) if p == 0 else pl.ds(base + (p - 1) * (n // 2), n // 2)

        x1, x2, x3 = ring_x((w, 0), lambda i, p: f_ref.at[jy, i, part(h1, p)], owns)
        y1, y2, y3 = ring_y((w, 1), lambda j, p: f_ref.at[j, :, part(h1, p)])
        v1, v2, v3 = ring_y((w, 2), lambda j, p: f_ref.at[j, x, part(h2, p)])
        u1, u2, u3 = ring_x((w, 3), lambda i, p: f_ref.at[:, i, part(h2, p)], None)

        def t0():
            wave_arrived(w)
            x1()
            v1()

        def t1():
            x2()
            v2()

        def t2():
            x3()
            v3()
            y1()
            u1()

        def t3():
            y2()
            u2()

        def t4():
            y3()
            u3()
            out(w).start()

        return t0, t1, t2, t3, t4

    for a in (4, 3, 2, 1):
        stride_step(1, a)
    cp.start(
        abuf.at[:, k], f_ref.at[jy, x, pl.ds(c * 4, 4)], other, zero_at, when=jnp.logical_not(owns)
    )
    ticks = [wave(w) for w in range(5)]
    for kind, n, m in SCHEDULE:
        if kind == "B":
            stride_step(int(n), int(m))
        else:
            ticks[int(n)][int(m)]()
    for w in range(5):
        out(w).wait()
    cp.drain()
    assert cp.used <= SEMS, cp.used


SCHEDULE = (
    ("w00", "B24", "B23", "B22", "w10", "w01", "B34")
    + ("B33", "w20", "w11", "w02", "B44", "w30", "w21", "w12", "w03")
    + ("w40", "w31", "w22", "w13", "w04", "w41", "w32", "w23", "w14")
    + ("w42", "w33", "w24", "w43", "w34", "w44")
)
SEMS = 120


def move(gate, up, down, gain):
    return pl.pallas_call(
        move_kernel,
        out_shape=jax.ShapeDtypeStruct((2, 4, 64, 24, 128), jnp.bfloat16),
        in_specs=[pl.BlockSpec(memory_space=pl.ANY)] * 3 + [pl.BlockSpec(memory_space=pltpu.VMEM)],
        out_specs=pl.BlockSpec(memory_space=pl.ANY),
        scratch_shapes=[
            pltpu.VMEM((3, 32, 32, 32), jnp.float32),
            pltpu.VMEM((2, 4, 64, 24, 128), jnp.bfloat16),
            pltpu.VMEM((4, 8, 24, 128), jnp.bfloat16),
            pltpu.VMEM((4, 8, 24, 128), jnp.bfloat16),
            pltpu.VMEM((2, 3, 3, 4, 24, 128), jnp.bfloat16),
            pltpu.SemaphoreType.DMA((3,)),
            pltpu.SemaphoreType.DMA((5,)),
            pltpu.SemaphoreType.DMA((SEMS,)),
            pltpu.SemaphoreType.DMA((SEMS,)),
        ],
        compiler_params=pltpu.CompilerParams(
            collective_id=0, has_side_effects=True, vmem_limit_bytes=56 << 20
        ),
    )(gate, up, down, gain)


def expert_kernel(
    f_hbm,
    prompt_ref,
    group_ref,
    inner_ref,
    weight_ref,
    turn_ref,
    gate_out,
    up_out,
    down_out,
    part_ref,
    f_ref,
    normed,
    gate_ref,
    up_ref,
    down_ref,
    load,
    sems,
):
    z = lax.axis_index("fs") // 2

    def fetch(w):
        slots = pl.ds(WAVE_AT[w], WAVE_N[w])
        return pltpu.make_async_copy(f_hbm.at[:, :, slots], f_ref.at[:, :, slots], load.at[w])

    for w in range(5):
        fetch(w).start()
    values = prompt_ref[...].astype(jnp.float32)
    normed[...] = (
        values * lax.rsqrt(jnp.mean(values * values, axis=1, keepdims=True) + 1e-06)
    ).astype(jnp.bfloat16)
    for w in range(5):
        fetch(w).wait()
        for j in (0, 1):
            at, n = WAVE_AT[w], WAVE_N[w]
            taken = [
                f_ref[j, i, at : at + n].astype(jnp.float32).reshape(n * 24, 128).astype(jnp.bfloat16)
                for i in range(4)
            ]
            turned = jnp.dot(
                jnp.concatenate(taken, axis=1), turn_ref[...], preferred_element_type=jnp.float32
            )
            for m in range(n):
                side, core, b, a = slot_source(w, m)
                source = lax.rem(z - 4 * a - (1 - 2 * core) * BVAL[b] + 64, 32)
                row = pl.multiple_of((source * 2 + core) * 32, 32)
                for k, out in enumerate((gate_ref, up_ref, down_ref)):
                    first = m * 24 + k * 8
                    rows = [turned[first : first + 8, 128 * q : 128 * q + 128] for q in range(4)]
                    out[pl.ds(row, 32), 128 * j : 128 * j + 128] = jnp.concatenate(
                        rows, axis=0
                    ).astype(jnp.bfloat16)
    stores = [
        pltpu.make_async_copy(a, b, sems.at[i])
        for i, (a, b) in enumerate(((gate_ref, gate_out), (up_ref, up_out), (down_ref, down_out)))
    ]
    for store in stores:
        store.start()
    gate_act = jnp.dot(normed[...], gate_ref[...], preferred_element_type=jnp.float32) * 2048 ** (-0.5)
    up_act = jnp.dot(normed[...], up_ref[...], preferred_element_type=jnp.float32) * 2048 ** (-0.5)
    chosen = group_ref[...] * EPG + inner_ref[...]
    row = jnp.sum(jnp.where(chosen == z, weight_ref[...], 0.0), axis=0, keepdims=True)
    column = jnp.broadcast_to(row, (8, 256)).T[:, :1]
    silu = gate_act / (1.0 + jnp.exp(-gate_act))
    scaled = (column * silu * up_act).astype(jnp.bfloat16)
    for n in range(8):
        part = lax.dot_general(
            down_ref[n * 256 : (n + 1) * 256],
            scaled,
            (((1,), (1,)), ((), ())),
            preferred_element_type=jnp.float32,
        ).astype(jnp.bfloat16)
        for i in range(8):
            owner = n * 8 + i
            part_ref[owner % 2, owner // 2 % 4, owner // 8] = part[i * 32 : (i + 1) * 32]
    for store in stores:
        store.wait()


def slot_source(w, m):
    if w in (0, 4):
        return 0, m // 4, m % 4, w
    side, rest = divmod(m, 8)
    return side, rest // 4, rest % 4, -w if side else w


EXPERT_VMEM = 51


def turning():
    at = np.arange(512).reshape(4, 4, 32).transpose(1, 0, 2).reshape(512)
    return np.eye(512, dtype=np.float32)[:, at]


def expert(moved, prompt, group, inner, weight):
    served = jax.ShapeDtypeStruct((2048, 256), jnp.bfloat16)
    vmem = pl.BlockSpec(memory_space=pltpu.VMEM)
    hbm = pl.BlockSpec(memory_space=pl.ANY)
    return pl.pallas_call(
        expert_kernel,
        out_shape=(served, served, served, jax.ShapeDtypeStruct((2, 4, 8, 32, 256), jnp.bfloat16)),
        in_specs=[hbm] + [vmem] * 5,
        out_specs=(hbm, hbm, hbm, vmem),
        scratch_shapes=[
            pltpu.VMEM((2, 4, 64, 24, 128), jnp.bfloat16),
            pltpu.VMEM((256, 2048), jnp.bfloat16),
            pltpu.VMEM((2048, 256), jnp.bfloat16),
            pltpu.VMEM((2048, 256), jnp.bfloat16),
            pltpu.VMEM((2048, 256), jnp.bfloat16),
            pltpu.SemaphoreType.DMA((5,)),
            pltpu.SemaphoreType.DMA((3,)),
        ],
        compiler_params=pltpu.CompilerParams(vmem_limit_bytes=EXPERT_VMEM << 20),
    )(moved, prompt, group, inner, weight, jnp.asarray(turning(), jnp.bfloat16))


FAR_FIRST = (4, 3, -3, 2, -2, 1, -1, 0)


def sum_kernel(p_ref, o_ref, xbuf, qbuf, abuf, ubuf, rbuf, tbuf, send, recv):
    z, c, y, x = place()
    s = 1 - 2 * c
    k = z // 4
    other = device(z, 1 - c, y, x)
    greet([device(z + d, c, y, x) for d in (1, -1, 2, -2, 4, -4)] + [other])
    cp = Copies(send, recv)

    def chunk(near, a):
        near = lax.rem(near + 32, 32)
        return lax.rem(near, 4), lax.rem(near // 4 + a + 8, 8)

    order = (3, 1, 2, 0)
    core_at = {}
    for a in FAR_FIRST:
        for i in order:
            q, at = chunk(z - BVAL[i] * s, a)
            core_at[a, i] = cp.slots()
            cp.start(p_ref.at[1 - c, q, at], xbuf.at[q, at], other, core_at[a, i])
    near_at = {}
    for a in FAR_FIRST:
        for i in order:
            q, at = chunk(z + BVAL[i] * s, a)
            cp.arrived(xbuf.at[q, at], other, core_at[a, i])
            n = (a + 8) % 8
            total = p_ref[c, q, at].astype(jnp.float32) + xbuf[q, at].astype(jnp.float32)
            qbuf[i, n] = total.astype(jnp.bfloat16)
            if i:
                near_at[a, i] = cp.slots()
                cp.start(
                    qbuf.at[i, n], abuf.at[i - 1, n], device(z + BVAL[i] * s, c, y, x), near_at[a, i]
                )

    def mine(a):
        at = (a + 8) % 8
        for i in (1, 2, 3):
            cp.arrived(abuf.at[i - 1, at], other, near_at[a, i])
        total = qbuf[0, at].astype(jnp.float32) + abuf[0, at].astype(jnp.float32)
        return total + (abuf[1, at].astype(jnp.float32) + abuf[2, at].astype(jnp.float32))

    via = (device(z + 4, c, y, x), device(z - 4, c, y, x))
    ring_at = [cp.slots(2) for _ in range(4)]
    ubuf[...] = mine(4).astype(jnp.bfloat16)
    for side in (0, 1):
        rows = pl.ds(16 * side, 16)
        cp.start(ubuf.at[rows], rbuf.at[side, 0, rows], via[side], ring_at[0] + side)
    for n in (1, 2, 3):
        held = [mine(4 - n), mine(n - 4)]
        for side in (0, 1):
            if n == 1:
                rows = pl.ds(16 * side, 16)
                cp.arrived(rbuf.at[side, 0, rows], other, ring_at[0] + side)
                came = rbuf[side, 0, 16 * side : 16 * side + 16].astype(jnp.float32)
                tbuf[side, 0, 16 * side : 16 * side + 16] = (
                    held[side][16 * side : 16 * side + 16] + came
                ).astype(jnp.bfloat16)
                tbuf[side, 0, 16 - 16 * side : 32 - 16 * side] = held[side][
                    16 - 16 * side : 32 - 16 * side
                ].astype(jnp.bfloat16)
            else:
                cp.arrived(rbuf.at[side, n - 1], other, ring_at[n - 1] + side)
                tbuf[side, n - 1] = (held[side] + rbuf[side, n - 1].astype(jnp.float32)).astype(
                    jnp.bfloat16
                )
            cp.start(tbuf.at[side, n - 1], rbuf.at[side, n], via[side], ring_at[n] + side)
    total = mine(0)
    for side in (0, 1):
        cp.arrived(rbuf.at[side, 3], other, ring_at[3] + side)
        total = total + rbuf[side, 3].astype(jnp.float32)
    o_ref[...] = (total * FF ** (-0.5)).astype(jnp.bfloat16)
    cp.drain()


def summed(parts):
    return pl.pallas_call(
        sum_kernel,
        out_shape=jax.ShapeDtypeStruct((32, 256), jnp.bfloat16),
        in_specs=[pl.BlockSpec(memory_space=pltpu.VMEM)],
        out_specs=pl.BlockSpec(memory_space=pltpu.VMEM),
        scratch_shapes=[
            pltpu.VMEM((4, 8, 32, 256), jnp.bfloat16),
            pltpu.VMEM((4, 8, 32, 256), jnp.bfloat16),
            pltpu.VMEM((3, 8, 32, 256), jnp.bfloat16),
            pltpu.VMEM((32, 256), jnp.bfloat16),
            pltpu.VMEM((2, 4, 32, 256), jnp.bfloat16),
            pltpu.VMEM((2, 3, 32, 256), jnp.bfloat16),
            pltpu.SemaphoreType.DMA((64,)),
            pltpu.SemaphoreType.DMA((64,)),
        ],
        compiler_params=pltpu.CompilerParams(
            collective_id=1, has_side_effects=True, vmem_limit_bytes=16 << 20
        ),
    )(parts)


def shards(
    prompt, norm_gain, gate_master, up_master, down_master, group_choice, inner_choice, route_weight
):
    moved = move(gate_master, up_master, down_master, norm_gain[None, :])
    gate, up, down, parts = expert(
        moved, prompt, group_choice[None, :], inner_choice.T, route_weight.T
    )
    return gate, up, down, summed(parts).T


def solution(mesh):
    in_specs = (
        P("tp", None),
        P("fs"),
        P(None, "fs", "tp"),
        P(None, "fs", "tp"),
        P(None, "fs", "tp"),
        P("tp"),
        P("tp", None),
        P("tp", None),
    )
    out_specs = (P(None, "fs"), P(None, "fs"), P(None, "fs"), P("tp", "fs"))
    return jax.shard_map(
        shards, mesh=mesh, in_specs=in_specs, out_specs=out_specs, check_vma=False
    )
```

```python
import jax
import jax.numpy as jnp
import numpy as np
from jax import lax
from jax.experimental import pallas as pl
from jax.experimental.pallas import tpu as pltpu
from jax.sharding import PartitionSpec as P

FF = 512
EPG = 8
MESH = pl.DeviceIdType.MESH
BVAL = (0, 1, -1, 2)
WAVE_AT = (0, 8, 24, 40, 56)
WAVE_N = (8, 16, 16, 16, 8)
FAR_FIRST = (4, 3, -3, 2, -2, 1, -1, 0)


def place():
    fs = lax.axis_index("fs")
    tp = lax.axis_index("tp")
    return fs // 2, fs % 2, tp // 4, tp % 4


def device(z, c, y, x):
    return {"fs": lax.rem(z + 32, 32) * 2 + c, "tp": lax.rem(y + 4, 4) * 4 + lax.rem(x + 4, 4)}


def chunk(near, a):
    near = lax.rem(near + 32, 32)
    return lax.rem(near, 4), lax.rem(near // 4 + a + 8, 8)


class Copies:
    def __init__(self, send, recv):
        self.send, self.recv, self.used, self.pending = send, recv, 0, []

    def slots(self, n=1):
        at = self.used
        self.used += n
        return at

    def make(self, src, dst, dev, at, to=0):
        return pltpu.make_async_remote_copy(
            src_ref=src,
            dst_ref=dst,
            send_sem=self.send.at[at],
            recv_sem=self.recv.at[at + to],
            device_id=dev,
            device_id_type=MESH,
        )

    def start(self, src, dst, dev, at, to=0, when=None):
        def go():
            self.make(src, dst, dev, at, to).start()

        def end():
            self.make(src, dst, dev, at, to).wait_send()

        if when is None:
            go()
        else:
            pl.when(when)(go)
        self.pending.append((when, end))

    def arrived(self, ref, dev, at, to=0):
        self.make(ref, ref, dev, at, to).wait_recv()

    def drain(self):
        for when, end in self.pending:
            if when is None:
                end()
            else:
                pl.when(when)(end)


def greet(partners, meanwhile=None):
    barrier = pltpu.get_barrier_semaphore()
    for dev in partners:
        pl.semaphore_signal(barrier, inc=1, device_id=dev, device_id_type=MESH)
    if meanwhile is not None:
        meanwhile()
    pl.semaphore_wait(barrier, len(partners))


def pack(gain_ref, held, s_ref, gain_load, loads):
    gain_load.wait()
    eye = lax.broadcasted_iota(jnp.int32, (32, 32), 0) == lax.broadcasted_iota(jnp.int32, (32, 32), 1)
    gain = jnp.sum(jnp.where(eye, gain_ref[...], 0.0), axis=1, keepdims=True)
    hidden = lax.broadcasted_iota(jnp.int32, (32, 128), 0)
    lane = lax.broadcasted_iota(jnp.int32, (32, 128), 1)
    for n, load in enumerate(loads):
        load.wait()
        total = jnp.zeros((256, 128), jnp.float32)
        for q in range(4):
            rows = held[n, :, 8 * q : 8 * q + 8, :]
            if n < 2:
                rows = rows * gain[8 * q : 8 * q + 8][None]
            place_q = (lane == hidden + 32 * q).astype(jnp.float32).astype(jnp.bfloat16)
            total += jnp.dot(
                rows.reshape(256, 32).astype(jnp.bfloat16), place_q, preferred_element_type=jnp.float32
            )
        for e in range(32):
            s_ref[e % 4, e // 4, 8 * n : 8 * n + 8] = total[8 * e : 8 * e + 8].astype(jnp.bfloat16)


def partners():
    z, c, y, x = place()
    near = [device(z + d, c, y, x) for d in (1, -1, 2, -2, 4, -4)]
    near += [device(z + d, 1 - c, y, x) for d in (4, -4)] + [device(z, 1 - c, y, x)]
    flat = ((0, 1), (0, -1), (1, 0), (-1, 0), (0, 2), (2, 0))
    return near + [device(z, c, y + b, x + a) for b, a in flat]


def move(cp, s_ref, abuf, bbuf, f_ref, settle, meanwhile):
    z, c, y, x = place()
    s = 1 - 2 * c
    owner = y // 2
    jy = y % 2
    rel = lax.rem(y - 2 * c + 4, 4)
    owns = rel < 2
    other = device(z, 1 - c, y, x)
    right, left = device(z, c, y, x + 1), device(z, c, y, x - 1)
    up, down = device(z, c, y + 1, x), device(z, c, y - 1, x)

    near_at = {}
    for a in FAR_FIRST:
        for i in (3, 1, 2):
            near = z + BVAL[i] * s
            q, at = chunk(near, a)
            near_at[a, i] = cp.slots()
            cp.start(s_ref.at[q, at], abuf.at[i, (a + 8) % 8], device(near, c, y, x), near_at[a, i])
    for a in FAR_FIRST:
        q, at = chunk(z, a)
        abuf[0, (a + 8) % 8] = s_ref[q, at]

    meanwhile()

    def near_arrived(a):
        for i in (1, 2, 3):
            cp.arrived(abuf.at[i, (a + 8) % 8], other, near_at[a, i])

    def slot(a, direction):
        w = abs(a)
        if w in (0, 4):
            return WAVE_AT[w] + c * 4
        return WAVE_AT[w] + (0 if direction > 0 else 8) + c * 4

    hop = {}
    final = {}

    def stride_step(n, a):
        for side, direction in ((0, 1), (1, -1)):
            via = device(z + 4 * direction, c, y, x)
            end = device(z + 4 * direction, owner, y, x)
            half = pl.ds(2 * side, 2) if a == 4 else pl.ds(0, 4)
            width = 2 if a == 4 else 4
            if n == 1:
                src = abuf.at[half, (direction * a + 8) % 8]
            else:
                src = bbuf.at[side, n - 2, a - 2, pl.ds(0, width)]
                cp.arrived(src, other, hop[side, n - 1, a])
            if a == n:
                at = cp.slots(2)
                first = slot(a, direction) + (2 * side if a == 4 else 0)
                cp.start(src, f_ref.at[jy, x, pl.ds(first, width)], end, at, c)
                final[side, a] = (at, width)
            else:
                at = cp.slots(1)
                hop[side, n, a] = at
                cp.start(src, bbuf.at[side, n - 1, a - 2, pl.ds(0, width)], via, at)

    zero_at = cp.slots(1)

    def wave_arrived(w):
        if w == 0:

            @pl.when(owns)
            def _():
                f_ref[jy, x, pl.ds(c * 4, 4)] = abuf[:, 0]
                cp.arrived(f_ref.at[jy, x, pl.ds((1 - c) * 4, 4)], other, zero_at)

            return

        @pl.when(owns)
        def _():
            for side in (0, 1):
                at, width = final[side, w]
                for core in (0, 1):
                    cp.arrived(f_ref.at[jy, x, pl.ds(0, width)], other, at, core)

    ring = {}

    def direct_x(key, take, when):
        def first():
            at = ring[key] = cp.slots(3)
            for n, d in enumerate((2, 1, 3)):
                cp.start(take(x, 0), take(x, 0), device(z, c, y, x + d), at + n, when=when)

        def second():
            def wait():
                for n, d in enumerate((2, 1, 3)):
                    cp.arrived(take(lax.rem(x + 4 - d, 4), 0), other, ring[key] + n)

            if when is None:
                wait()
            else:
                pl.when(when)(wait)

        return first, second

    def direct_y(key, take):
        def first():
            at = ring[key] = cp.slots(3)
            for n, d in enumerate((2, 1, 3)):
                cp.start(take(jy, 0), take(jy, 0), device(z, c, y + d, x), at + n, when=owns)

        def second():
            at = ring[key]

            @pl.when(plus)
            def _():
                cp.arrived(take(got, 0), other, at + 1)

            @pl.when(minus)
            def _():
                cp.arrived(take(got, 0), other, at + 2)

            @pl.when(jnp.logical_not(owns))
            def _():
                cp.arrived(take(jy, 0), other, at)

        return first, second

    def ring_x(key, take, when):
        def first():
            at = ring[key] = cp.slots(4)
            cp.start(take(x, 0), take(x, 0), right, at, when=when)
            cp.start(take(x, 0), take(x, 0), left, at + 1, when=when)

        def second():
            at = ring[key]

            def wait():
                cp.arrived(take(lax.rem(x + 3, 4), 0), other, at)
                cp.arrived(take(lax.rem(x + 1, 4), 0), other, at + 1)

            if when is None:
                wait()
            else:
                pl.when(when)(wait)
            cp.start(take(lax.rem(x + 3, 4), 1), take(lax.rem(x + 3, 4), 1), right, at + 2, when=when)
            cp.start(take(lax.rem(x + 1, 4), 2), take(lax.rem(x + 1, 4), 2), left, at + 3, when=when)

        def last():
            at = ring[key]

            def wait():
                cp.arrived(take(lax.rem(x + 2, 4), 1), other, at + 2)
                cp.arrived(take(lax.rem(x + 2, 4), 2), other, at + 3)

            if when is None:
                wait()
            else:
                pl.when(when)(wait)

        return first, second, last

    plus = (rel == 1) | (rel == 2)
    minus = (rel == 0) | (rel == 3)
    got = 1 - lax.rem(rel, 2)

    def ring_y(key, take):
        def first():
            at = ring[key] = cp.slots(4)
            cp.start(take(jy, 0), take(jy, 0), up, at, when=owns)
            cp.start(take(jy, 0), take(jy, 0), down, at + 1, when=owns)

        def second():
            at = ring[key]

            @pl.when(plus)
            def _():
                cp.arrived(take(got, 0), other, at)

            @pl.when(minus)
            def _():
                cp.arrived(take(got, 0), other, at + 1)

            cp.start(take(got, 1), take(got, 1), up, at + 2, when=plus)
            cp.start(take(got, 2), take(got, 2), down, at + 3, when=minus)

        def last():
            at = ring[key]

            @pl.when(jnp.logical_not(owns))
            def _():
                cp.arrived(take(jy, 1), other, at + 2)
                cp.arrived(take(jy, 2), other, at + 3)

        return first, second, last

    def wave(w):
        n = WAVE_N[w] // 2
        h1, h2 = WAVE_AT[w], WAVE_AT[w] + n

        def part(base, p):
            return pl.ds(base, n) if p == 0 else pl.ds(base + (p - 1) * (n // 2), n // 2)

        views = (
            lambda i, p: f_ref.at[jy, i, part(h1, p)],
            lambda j, p: f_ref.at[j, :, part(h1, p)],
            lambda j, p: f_ref.at[j, x, part(h2, p)],
            lambda i, p: f_ref.at[:, i, part(h2, p)],
        )
        if w in DIRECT:
            x1, x2 = direct_x((w, 0), views[0], owns)
            y1, y2 = direct_y((w, 1), views[1])
            v1, v2 = direct_y((w, 2), views[2])
            u1, u2 = direct_x((w, 3), views[3], None)

            def d0():
                wave_arrived(w)
                x1()
                v1()

            def d1():
                x2()
                y1()
                v2()
                u1()

            def d2():
                y2()
                u2()
                settle(w)

            return d0, d1, d2
        x1, x2, x3 = ring_x((w, 0), views[0], owns)
        y1, y2, y3 = ring_y((w, 1), views[1])
        v1, v2, v3 = ring_y((w, 2), views[2])
        u1, u2, u3 = ring_x((w, 3), views[3], None)

        def t0():
            wave_arrived(w)
            x1()
            v1()

        def t1():
            x2()
            v2()

        def t2():
            x3()
            v3()
            y1()
            u1()

        def t3():
            y2()
            u2()

        def t4():
            y3()
            u3()
            settle(w)

        return t0, t1, t2, t3, t4

    for a in (4, 3, 2, 1):
        near_arrived(a)
        if a < 4:
            near_arrived(-a)
        stride_step(1, a)
    near_arrived(0)
    cp.start(
        abuf.at[:, 0], f_ref.at[jy, x, pl.ds(c * 4, 4)], other, zero_at, when=jnp.logical_not(owns)
    )
    ticks = [wave(w) for w in range(5)]
    for kind, n, m in SCHEDULE:
        if kind == "B":
            stride_step(int(n), int(m))
        else:
            ticks[int(n)][int(m)]()


DIRECT = (4,)
SCHEDULE = (
    ("w00", "B24", "B23", "B22", "w10", "w01", "B34")
    + ("B33", "w20", "w11", "w02", "B44", "w30", "w21", "w12", "w03")
    + ("w40", "w31", "w22", "w13", "w04", "w41", "w32", "w23", "w14")
    + ("w42", "w33", "w24", "w34")
)
SEMS = 208


def slot_source(w, m):
    if w in (0, 4):
        return 0, m // 4, m % 4, w
    side, rest = divmod(m, 8)
    return side, rest // 4, rest % 4, -w if side else w


def turning():
    at = np.arange(512).reshape(4, 4, 32).transpose(1, 0, 2).reshape(512)
    return np.eye(512, dtype=np.float32)[:, at]


def settle_wave(w, z, f_ref, turn_ref, served):
    at, n = WAVE_AT[w], WAVE_N[w]
    for j in (0, 1):
        taken = [
            f_ref[j, i, at : at + n].astype(jnp.float32).reshape(n * 24, 128).astype(jnp.bfloat16)
            for i in range(4)
        ]
        turned = jnp.dot(
            jnp.concatenate(taken, axis=1), turn_ref[...], preferred_element_type=jnp.float32
        )
        for m in range(n):
            side, core, b, a = slot_source(w, m)
            source = lax.rem(z - 4 * a - (1 - 2 * core) * BVAL[b] + 64, 32)
            row = pl.multiple_of((source * 2 + core) * 32, 32)
            for k in range(3):
                first = m * 24 + k * 8
                rows = [turned[first : first + 8, 128 * q : 128 * q + 128] for q in range(4)]
                served[k, pl.ds(row, 32), 128 * j : 128 * j + 128] = jnp.concatenate(
                    rows, axis=0
                ).astype(jnp.bfloat16)


def partial_sums(z, normed, served, group_ref, inner_ref, weight_ref, part_ref):
    gate_act = jnp.dot(normed[...], served[0], preferred_element_type=jnp.float32) * 2048 ** (-0.5)
    up_act = jnp.dot(normed[...], served[1], preferred_element_type=jnp.float32) * 2048 ** (-0.5)
    chosen = group_ref[...] * EPG + inner_ref[...]
    row = jnp.sum(jnp.where(chosen == z, weight_ref[...], 0.0), axis=0, keepdims=True)
    column = jnp.broadcast_to(row, (8, 256)).T[:, :1]
    silu = gate_act / (1.0 + jnp.exp(-gate_act))
    scaled = (column * silu * up_act).astype(jnp.bfloat16)
    for n in range(8):
        part = lax.dot_general(
            served[2, n * 256 : (n + 1) * 256],
            scaled,
            (((1,), (1,)), ((), ())),
            preferred_element_type=jnp.float32,
        ).astype(jnp.bfloat16)
        for i in range(8):
            owner = n * 8 + i
            part_ref[owner % 2, owner // 2 % 4, owner // 8] = part[i * 32 : (i + 1) * 32]


def sum_parts(cp, p_ref, o_ref, xbuf, qbuf, abuf, ubuf, rbuf, tbuf):
    z, c, y, x = place()
    s = 1 - 2 * c
    other = device(z, 1 - c, y, x)
    order = (3, 1, 2, 0)
    core_at = {}
    for a in FAR_FIRST:
        for i in order:
            q, at = chunk(z - BVAL[i] * s, a)
            core_at[a, i] = cp.slots()
            cp.start(p_ref.at[1 - c, q, at], xbuf.at[q, at], other, core_at[a, i])
    near_at = {}
    for a in FAR_FIRST:
        for i in order:
            q, at = chunk(z + BVAL[i] * s, a)
            cp.arrived(xbuf.at[q, at], other, core_at[a, i])
            n = (a + 8) % 8
            total = p_ref[c, q, at].astype(jnp.float32) + xbuf[q, at].astype(jnp.float32)
            qbuf[i, n] = total.astype(jnp.bfloat16)
            if i:
                near_at[a, i] = cp.slots()
                cp.start(
                    qbuf.at[i, n], abuf.at[i - 1, n], device(z + BVAL[i] * s, c, y, x), near_at[a, i]
                )

    def mine(a):
        at = (a + 8) % 8
        for i in (1, 2, 3):
            cp.arrived(abuf.at[i - 1, at], other, near_at[a, i])
        total = qbuf[0, at].astype(jnp.float32) + abuf[0, at].astype(jnp.float32)
        return total + (abuf[1, at].astype(jnp.float32) + abuf[2, at].astype(jnp.float32))

    via = (device(z + 4, c, y, x), device(z - 4, c, y, x))
    ring_at = [cp.slots(4) for _ in range(4)]

    def onward(n, side, h, source):
        rows = pl.ds(16 * h, 16)
        cp.start(source, rbuf.at[side, n, rows], via[side], ring_at[n] + 2 * side + h)

    def came(n, side, h):
        rows = pl.ds(16 * h, 16)
        cp.arrived(rbuf.at[side, n, rows], other, ring_at[n] + 2 * side + h)
        return rbuf[side, n, 16 * h : 16 * h + 16].astype(jnp.float32)

    ubuf[...] = mine(4).astype(jnp.bfloat16)
    for side in (0, 1):
        onward(0, side, side, ubuf.at[pl.ds(16 * side, 16)])
    for n in (1, 2, 3):
        held = [mine(4 - n), mine(n - 4)]
        for order in (0, 1):
            for side in (0, 1):
                h = side if order == (0 if n > 1 else 1) else 1 - side
                total = held[side][16 * h : 16 * h + 16]
                if n > 1 or h == side:
                    total = total + came(n - 1, side, h)
                tbuf[side, n - 1, 16 * h : 16 * h + 16] = total.astype(jnp.bfloat16)
                onward(n, side, h, tbuf.at[side, n - 1, pl.ds(16 * h, 16)])
    total = mine(0)
    sums = [
        total[16 * h : 16 * h + 16] + came(3, h, h) + came(3, 1 - h, h) for h in (0, 1)
    ]
    total = jnp.concatenate(sums, axis=0)
    o_ref[...] = (total * FF ** (-0.5)).astype(jnp.bfloat16)


def whole_kernel(
    gate_hbm,
    up_hbm,
    down_hbm,
    gain_hbm,
    prompt_hbm,
    group_hbm,
    inner_hbm,
    weight_hbm,
    turn_hbm,
    gate_out,
    up_out,
    down_out,
    o_ref,
    held,
    gain,
    prompt,
    group,
    inner,
    weight,
    turn,
    s_ref,
    abuf,
    bbuf,
    f_ref,
    normed,
    served,
    part,
    xbuf,
    qbuf,
    nbuf,
    ubuf,
    rbuf,
    tbuf,
    load,
    store,
    send,
    recv,
):
    z = lax.axis_index("fs") // 2
    pairs = (
        (gain_hbm, gain),
        (gate_hbm, held.at[0]),
        (up_hbm, held.at[1]),
        (down_hbm, held.at[2]),
        (prompt_hbm, prompt),
        (turn_hbm, turn),
        (group_hbm, group),
        (inner_hbm, inner),
        (weight_hbm, weight),
    )
    loads = [pltpu.make_async_copy(a, b, load.at[n]) for n, (a, b) in enumerate(pairs)]
    stores = [
        pltpu.make_async_copy(served.at[n], out, store.at[n])
        for n, out in enumerate((gate_out, up_out, down_out))
    ]

    def ready():
        for copy in loads:
            copy.start()
        pack(gain, held, s_ref, loads[0], loads[1:4])

    def meanwhile():
        for copy in loads[4:]:
            copy.wait()
        values = prompt[...].astype(jnp.float32)
        normed[...] = (
            values * lax.rsqrt(jnp.mean(values * values, axis=1, keepdims=True) + 1e-06)
        ).astype(jnp.bfloat16)

    greet(partners(), ready)
    cp = Copies(send, recv)
    move(
        cp, s_ref, abuf, bbuf, f_ref, lambda w: settle_wave(w, z, f_ref, turn, served), meanwhile
    )
    for copy in stores:
        copy.start()
    partial_sums(z, normed, served, group, inner, weight, part)
    sum_parts(cp, part, o_ref, xbuf, qbuf, nbuf, ubuf, rbuf, tbuf)
    for copy in stores:
        copy.wait()
    cp.drain()
    assert cp.used <= SEMS, cp.used


def whole(gate, up, down, gain, prompt, group, inner, weight):
    hbm = pl.BlockSpec(memory_space=pl.ANY)
    out = jax.ShapeDtypeStruct((2048, 256), jnp.bfloat16)
    bf16, f32 = jnp.bfloat16, jnp.float32
    return pl.pallas_call(
        whole_kernel,
        out_shape=(out, out, out, jax.ShapeDtypeStruct((32, 256), bf16)),
        in_specs=[hbm] * 9,
        out_specs=(hbm, hbm, hbm, pl.BlockSpec(memory_space=pltpu.VMEM)),
        scratch_shapes=[
            pltpu.VMEM((3, 32, 32, 32), f32),
            pltpu.VMEM((1, 32), f32),
            pltpu.VMEM((256, 2048), bf16),
            pltpu.VMEM((1, 256), jnp.int32),
            pltpu.VMEM((2, 256), jnp.int32),
            pltpu.VMEM((2, 256), f32),
            pltpu.VMEM((512, 512), bf16),
            pltpu.VMEM((4, 8, 24, 128), bf16),
            pltpu.VMEM((4, 8, 24, 128), bf16),
            pltpu.VMEM((2, 3, 3, 4, 24, 128), bf16),
            pltpu.VMEM((2, 4, 64, 24, 128), bf16),
            pltpu.VMEM((256, 2048), bf16),
            pltpu.VMEM((3, 2048, 256), bf16),
            pltpu.VMEM((2, 4, 8, 32, 256), bf16),
            pltpu.VMEM((4, 8, 32, 256), bf16),
            pltpu.VMEM((4, 8, 32, 256), bf16),
            pltpu.VMEM((3, 8, 32, 256), bf16),
            pltpu.VMEM((32, 256), bf16),
            pltpu.VMEM((2, 4, 32, 256), bf16),
            pltpu.VMEM((2, 3, 32, 256), bf16),
            pltpu.SemaphoreType.DMA((9,)),
            pltpu.SemaphoreType.DMA((3,)),
            pltpu.SemaphoreType.DMA((SEMS,)),
            pltpu.SemaphoreType.DMA((SEMS,)),
        ],
        compiler_params=pltpu.CompilerParams(
            collective_id=0, has_side_effects=True, vmem_limit_bytes=58 << 20
        ),
    )(gate, up, down, gain, prompt, group, inner, weight, jnp.asarray(turning(), bf16))


def shards(
    prompt, norm_gain, gate_master, up_master, down_master, group_choice, inner_choice, route_weight
):
    gate, up, down, mixed = whole(
        gate_master,
        up_master,
        down_master,
        norm_gain[None, :],
        prompt,
        group_choice[None, :],
        inner_choice.T,
        route_weight.T,
    )
    return gate, up, down, mixed.T


def solution(mesh):
    in_specs = (
        P("tp", None),
        P("fs"),
        P(None, "fs", "tp"),
        P(None, "fs", "tp"),
        P(None, "fs", "tp"),
        P("tp"),
        P("tp", None),
        P("tp", None),
    )
    out_specs = (P(None, "fs"), P(None, "fs"), P(None, "fs"), P("tp", "fs"))
    return jax.shard_map(
        shards, mesh=mesh, in_specs=in_specs, out_specs=out_specs, check_vma=False
    )
```

```python
import jax
import jax.numpy as jnp
import numpy as np
from jax import lax
from jax.experimental import pallas as pl
from jax.experimental.pallas import tpu as pltpu
from jax.sharding import PartitionSpec as P

FF = 512
EPG = 8
MESH = pl.DeviceIdType.MESH
BVAL = (0, 1, -1, 2)
WAVE_AT = (0, 8, 24, 40, 56)
WAVE_N = (8, 16, 16, 16, 8)
FAR_FIRST = (4, 3, -3, 2, -2, 1, -1, 0)


def place():
    fs = lax.axis_index("fs")
    tp = lax.axis_index("tp")
    return fs // 2, fs % 2, tp // 4, tp % 4


def device(z, c, y, x):
    return {"fs": lax.rem(z + 32, 32) * 2 + c, "tp": lax.rem(y + 4, 4) * 4 + lax.rem(x + 4, 4)}


def chunk(near, a):
    near = lax.rem(near + 32, 32)
    return lax.rem(near, 4), lax.rem(near // 4 + a + 8, 8)


class Copies:
    def __init__(self, send, recv):
        self.send, self.recv, self.used, self.pending = send, recv, 0, []

    def slots(self, n=1):
        at = self.used
        self.used += n
        return at

    def make(self, src, dst, dev, at, to=0):
        return pltpu.make_async_remote_copy(
            src_ref=src,
            dst_ref=dst,
            send_sem=self.send.at[at],
            recv_sem=self.recv.at[at + to],
            device_id=dev,
            device_id_type=MESH,
        )

    def start(self, src, dst, dev, at, to=0, when=None):
        def go():
            self.make(src, dst, dev, at, to).start()

        def end():
            self.make(src, dst, dev, at, to).wait_send()

        if when is None:
            go()
        else:
            pl.when(when)(go)
        self.pending.append((when, end))

    def arrived(self, ref, dev, at, to=0):
        self.make(ref, ref, dev, at, to).wait_recv()

    def drain(self):
        for when, end in self.pending:
            if when is None:
                end()
            else:
                pl.when(when)(end)


def greet(partners, meanwhile=None):
    barrier = pltpu.get_barrier_semaphore()
    for dev in partners:
        pl.semaphore_signal(barrier, inc=1, device_id=dev, device_id_type=MESH)
    if meanwhile is not None:
        meanwhile()
    pl.semaphore_wait(barrier, len(partners))


def pack(gain_ref, held, s_ref, gain_load, loads):
    gain_load.wait()
    eye = lax.broadcasted_iota(jnp.int32, (32, 32), 0) == lax.broadcasted_iota(jnp.int32, (32, 32), 1)
    gain = jnp.sum(jnp.where(eye, gain_ref[...], 0.0), axis=1, keepdims=True)
    hidden = lax.broadcasted_iota(jnp.int32, (32, 128), 0)
    lane = lax.broadcasted_iota(jnp.int32, (32, 128), 1)
    for n, load in enumerate(loads):
        load.wait()
        total = jnp.zeros((256, 128), jnp.float32)
        for q in range(4):
            rows = held[n, :, 8 * q : 8 * q + 8, :]
            if n < 2:
                rows = rows * gain[8 * q : 8 * q + 8][None]
            place_q = (lane == hidden + 32 * q).astype(jnp.float32).astype(jnp.bfloat16)
            total += jnp.dot(
                rows.reshape(256, 32).astype(jnp.bfloat16), place_q, preferred_element_type=jnp.float32
            )
        for e in range(32):
            s_ref[e % 4, e // 4, 8 * n : 8 * n + 8] = total[8 * e : 8 * e + 8].astype(jnp.bfloat16)


def partners():
    z, c, y, x = place()
    near = [device(z + d, c, y, x) for d in (1, -1, 2, -2, 4, -4)]
    near += [device(z + d, 1 - c, y, x) for d in (4, -4)] + [device(z, 1 - c, y, x)]
    flat = ((0, 1), (0, -1), (1, 0), (-1, 0), (0, 2), (2, 0))
    return near + [device(z, c, y + b, x + a) for b, a in flat]


def move(cp, s_ref, abuf, bbuf, f_ref, settle, meanwhile):
    z, c, y, x = place()
    s = 1 - 2 * c
    owner = y // 2
    jy = y % 2
    rel = lax.rem(y - 2 * c + 4, 4)
    owns = rel < 2
    other = device(z, 1 - c, y, x)
    right, left = device(z, c, y, x + 1), device(z, c, y, x - 1)
    up, down = device(z, c, y + 1, x), device(z, c, y - 1, x)

    near_at = {}
    for a in FAR_FIRST:
        for i in (3, 1, 2):
            near = z + BVAL[i] * s
            q, at = chunk(near, a)
            near_at[a, i] = cp.slots()
            cp.start(s_ref.at[q, at], abuf.at[i, (a + 8) % 8], device(near, c, y, x), near_at[a, i])
    for a in FAR_FIRST:
        q, at = chunk(z, a)
        abuf[0, (a + 8) % 8] = s_ref[q, at]

    meanwhile()

    def near_arrived(a):
        for i in (1, 2, 3):
            cp.arrived(abuf.at[i, (a + 8) % 8], other, near_at[a, i])

    def slot(a, direction):
        w = abs(a)
        if w in (0, 4):
            return WAVE_AT[w] + c * 4
        return WAVE_AT[w] + (0 if direction > 0 else 8) + c * 4

    hop = {}
    final = {}

    def stride_step(n, a):
        for side, direction in ((0, 1), (1, -1)):
            via = device(z + 4 * direction, c, y, x)
            end = device(z + 4 * direction, owner, y, x)
            half = pl.ds(2 * side, 2) if a == 4 else pl.ds(0, 4)
            width = 2 if a == 4 else 4
            if n == 1:
                src = abuf.at[half, (direction * a + 8) % 8]
            else:
                src = bbuf.at[side, n - 2, a - 2, pl.ds(0, width)]
                cp.arrived(src, other, hop[side, n - 1, a])
            if a == n:
                at = cp.slots(2)
                first = slot(a, direction) + (2 * side if a == 4 else 0)
                cp.start(src, f_ref.at[jy, x, pl.ds(first, width)], end, at, c)
                final[side, a] = (at, width)
            else:
                at = cp.slots(1)
                hop[side, n, a] = at
                cp.start(src, bbuf.at[side, n - 1, a - 2, pl.ds(0, width)], via, at)

    zero_at = cp.slots(1)

    def wave_arrived(w):
        if w == 0:

            @pl.when(owns)
            def _():
                f_ref[jy, x, pl.ds(c * 4, 4)] = abuf[:, 0]
                cp.arrived(f_ref.at[jy, x, pl.ds((1 - c) * 4, 4)], other, zero_at)

            return

        @pl.when(owns)
        def _():
            for side in (0, 1):
                at, width = final[side, w]
                for core in (0, 1):
                    cp.arrived(f_ref.at[jy, x, pl.ds(0, width)], other, at, core)

    ring = {}

    def direct_x(key, take, when):
        def first():
            at = ring[key] = cp.slots(3)
            for n, d in enumerate((2, 1, 3)):
                cp.start(take(x, 0), take(x, 0), device(z, c, y, x + d), at + n, when=when)

        def second():
            def wait():
                for n, d in enumerate((2, 1, 3)):
                    cp.arrived(take(lax.rem(x + 4 - d, 4), 0), other, ring[key] + n)

            if when is None:
                wait()
            else:
                pl.when(when)(wait)

        return first, second

    def direct_y(key, take):
        def first():
            at = ring[key] = cp.slots(3)
            for n, d in enumerate((2, 1, 3)):
                cp.start(take(jy, 0), take(jy, 0), device(z, c, y + d, x), at + n, when=owns)

        def second():
            at = ring[key]

            @pl.when(plus)
            def _():
                cp.arrived(take(got, 0), other, at + 1)

            @pl.when(minus)
            def _():
                cp.arrived(take(got, 0), other, at + 2)

            @pl.when(jnp.logical_not(owns))
            def _():
                cp.arrived(take(jy, 0), other, at)

        return first, second

    def ring_x(key, take, when):
        def first():
            at = ring[key] = cp.slots(4)
            cp.start(take(x, 0), take(x, 0), right, at, when=when)
            cp.start(take(x, 0), take(x, 0), left, at + 1, when=when)

        def second():
            at = ring[key]

            def wait():
                cp.arrived(take(lax.rem(x + 3, 4), 0), other, at)
                cp.arrived(take(lax.rem(x + 1, 4), 0), other, at + 1)

            if when is None:
                wait()
            else:
                pl.when(when)(wait)
            cp.start(take(lax.rem(x + 3, 4), 1), take(lax.rem(x + 3, 4), 1), right, at + 2, when=when)
            cp.start(take(lax.rem(x + 1, 4), 2), take(lax.rem(x + 1, 4), 2), left, at + 3, when=when)

        def last():
            at = ring[key]

            def wait():
                cp.arrived(take(lax.rem(x + 2, 4), 1), other, at + 2)
                cp.arrived(take(lax.rem(x + 2, 4), 2), other, at + 3)

            if when is None:
                wait()
            else:
                pl.when(when)(wait)

        return first, second, last

    plus = (rel == 1) | (rel == 2)
    minus = (rel == 0) | (rel == 3)
    got = 1 - lax.rem(rel, 2)

    def ring_y(key, take):
        def first():
            at = ring[key] = cp.slots(4)
            cp.start(take(jy, 0), take(jy, 0), up, at, when=owns)
            cp.start(take(jy, 0), take(jy, 0), down, at + 1, when=owns)

        def second():
            at = ring[key]

            @pl.when(plus)
            def _():
                cp.arrived(take(got, 0), other, at)

            @pl.when(minus)
            def _():
                cp.arrived(take(got, 0), other, at + 1)

            cp.start(take(got, 1), take(got, 1), up, at + 2, when=plus)
            cp.start(take(got, 2), take(got, 2), down, at + 3, when=minus)

        def last():
            at = ring[key]

            @pl.when(jnp.logical_not(owns))
            def _():
                cp.arrived(take(jy, 1), other, at + 2)
                cp.arrived(take(jy, 2), other, at + 3)

        return first, second, last

    def wave(w):
        n = WAVE_N[w] // 2
        h1, h2 = WAVE_AT[w], WAVE_AT[w] + n

        def part(base, p):
            return pl.ds(base, n) if p == 0 else pl.ds(base + (p - 1) * (n // 2), n // 2)

        views = (
            lambda i, p: f_ref.at[jy, i, part(h1, p)],
            lambda j, p: f_ref.at[j, :, part(h1, p)],
            lambda j, p: f_ref.at[j, x, part(h2, p)],
            lambda i, p: f_ref.at[:, i, part(h2, p)],
        )
        if w in DIRECT:
            x1, x2 = direct_x((w, 0), views[0], owns)
            y1, y2 = direct_y((w, 1), views[1])
            v1, v2 = direct_y((w, 2), views[2])
            u1, u2 = direct_x((w, 3), views[3], None)

            def d0():
                wave_arrived(w)
                x1()
                v1()

            def d1():
                x2()
                y1()
                v2()
                u1()

            def d2():
                y2()
                u2()

            return d0, d1, d2
        x1, x2, x3 = ring_x((w, 0), views[0], owns)
        y1, y2, y3 = ring_y((w, 1), views[1])
        v1, v2, v3 = ring_y((w, 2), views[2])
        u1, u2, u3 = ring_x((w, 3), views[3], None)

        def t0():
            wave_arrived(w)
            x1()
            v1()

        def t1():
            x2()
            v2()

        def t2():
            x3()
            v3()
            y1()
            u1()

        def t3():
            y2()
            u2()

        def t4():
            y3()
            u3()

        return t0, t1, t2, t3, t4

    for a in (4, 3, 2, 1):
        near_arrived(a)
        if a < 4:
            near_arrived(-a)
        stride_step(1, a)
    near_arrived(0)
    cp.start(
        abuf.at[:, 0], f_ref.at[jy, x, pl.ds(c * 4, 4)], other, zero_at, when=jnp.logical_not(owns)
    )
    ticks = [wave(w) for w in range(5)]
    for kind, n, m in SCHEDULE:
        if kind == "B":
            stride_step(int(n), int(m))
        elif kind == "S":
            settle(int(n))
        else:
            ticks[int(n)][int(m)]()


DIRECT = (4,)
SCHEDULE = (
    ("w00", "B24", "B23", "B22", "w10", "w01", "B34")
    + ("B33", "w20", "w11", "w02", "B44", "w30", "w21", "w12", "w03")
    + ("w40", "w31", "w22", "w13", "w04", "w41", "w32", "w23", "S0.")
    + ("w14", "S1.", "w33", "w24", "S2.", "w42", "S4.", "w34", "S3.")
)
SEMS = 208


def slot_source(w, m):
    if w in (0, 4):
        return 0, m // 4, m % 4, w
    side, rest = divmod(m, 8)
    return side, rest // 4, rest % 4, -w if side else w


def turning():
    at = np.arange(512).reshape(4, 4, 32).transpose(1, 0, 2).reshape(512)
    return np.eye(512, dtype=np.float32)[:, at]


def settle_wave(w, z, f_ref, turn_ref, served):
    at, n = WAVE_AT[w], WAVE_N[w]
    for j in (0, 1):
        taken = [
            f_ref[j, i, at : at + n].astype(jnp.float32).reshape(n * 24, 128).astype(jnp.bfloat16)
            for i in range(4)
        ]
        turned = jnp.dot(
            jnp.concatenate(taken, axis=1), turn_ref[...], preferred_element_type=jnp.float32
        )
        for m in range(n):
            side, core, b, a = slot_source(w, m)
            source = lax.rem(z - 4 * a - (1 - 2 * core) * BVAL[b] + 64, 32)
            row = pl.multiple_of((source * 2 + core) * 32, 32)
            for k in range(3):
                first = m * 24 + k * 8
                rows = [turned[first : first + 8, 128 * q : 128 * q + 128] for q in range(4)]
                served[k, pl.ds(row, 32), 128 * j : 128 * j + 128] = jnp.concatenate(
                    rows, axis=0
                ).astype(jnp.bfloat16)


def partial_sums(z, normed, served, group_ref, inner_ref, weight_ref, part_ref):
    gate_act = jnp.dot(normed[...], served[0], preferred_element_type=jnp.float32) * 2048 ** (-0.5)
    up_act = jnp.dot(normed[...], served[1], preferred_element_type=jnp.float32) * 2048 ** (-0.5)
    chosen = group_ref[...] * EPG + inner_ref[...]
    row = jnp.sum(jnp.where(chosen == z, weight_ref[...], 0.0), axis=0, keepdims=True)
    column = jnp.broadcast_to(row, (8, 256)).T[:, :1]
    silu = gate_act / (1.0 + jnp.exp(-gate_act))
    scaled = (column * silu * up_act).astype(jnp.bfloat16)
    for n in range(8):
        part = lax.dot_general(
            served[2, n * 256 : (n + 1) * 256],
            scaled,
            (((1,), (1,)), ((), ())),
            preferred_element_type=jnp.float32,
        ).astype(jnp.bfloat16)
        for i in range(8):
            owner = n * 8 + i
            part_ref[owner % 2, owner // 2 % 4, owner // 8] = part[i * 32 : (i + 1) * 32]


def sum_parts(cp, p_ref, o_ref, xbuf, qbuf, abuf, ubuf, rbuf, tbuf):
    z, c, y, x = place()
    s = 1 - 2 * c
    other = device(z, 1 - c, y, x)
    order = (3, 1, 2, 0)
    core_at = {}
    for a in FAR_FIRST:
        for i in order:
            q, at = chunk(z - BVAL[i] * s, a)
            core_at[a, i] = cp.slots()
            cp.start(p_ref.at[1 - c, q, at], xbuf.at[q, at], other, core_at[a, i])
    near_at = {}
    for a in FAR_FIRST:
        for i in order:
            q, at = chunk(z + BVAL[i] * s, a)
            cp.arrived(xbuf.at[q, at], other, core_at[a, i])
            n = (a + 8) % 8
            total = p_ref[c, q, at].astype(jnp.float32) + xbuf[q, at].astype(jnp.float32)
            qbuf[i, n] = total.astype(jnp.bfloat16)
            if i:
                near_at[a, i] = cp.slots()
                cp.start(
                    qbuf.at[i, n], abuf.at[i - 1, n], device(z + BVAL[i] * s, c, y, x), near_at[a, i]
                )

    def mine(a):
        at = (a + 8) % 8
        for i in (1, 2, 3):
            cp.arrived(abuf.at[i - 1, at], other, near_at[a, i])
        total = qbuf[0, at].astype(jnp.float32) + abuf[0, at].astype(jnp.float32)
        return total + (abuf[1, at].astype(jnp.float32) + abuf[2, at].astype(jnp.float32))

    via = (device(z + 4, c, y, x), device(z - 4, c, y, x))
    ring_at = [cp.slots(4) for _ in range(4)]

    def onward(n, side, h, source):
        rows = pl.ds(16 * h, 16)
        cp.start(source, rbuf.at[side, n, rows], via[side], ring_at[n] + 2 * side + h)

    def came(n, side, h):
        rows = pl.ds(16 * h, 16)
        cp.arrived(rbuf.at[side, n, rows], other, ring_at[n] + 2 * side + h)
        return rbuf[side, n, 16 * h : 16 * h + 16].astype(jnp.float32)

    ubuf[...] = mine(4).astype(jnp.bfloat16)
    for side in (0, 1):
        onward(0, side, side, ubuf.at[pl.ds(16 * side, 16)])
    for n in (1, 2, 3):
        held = [mine(4 - n), mine(n - 4)]
        for order in (0, 1):
            for side in (0, 1):
                h = side if order == (0 if n > 1 else 1) else 1 - side
                total = held[side][16 * h : 16 * h + 16]
                if n > 1 or h == side:
                    total = total + came(n - 1, side, h)
                tbuf[side, n - 1, 16 * h : 16 * h + 16] = total.astype(jnp.bfloat16)
                onward(n, side, h, tbuf.at[side, n - 1, pl.ds(16 * h, 16)])
    total = mine(0)
    sums = [
        total[16 * h : 16 * h + 16] + came(3, h, h) + came(3, 1 - h, h) for h in (0, 1)
    ]
    total = jnp.concatenate(sums, axis=0)
    o_ref[...] = (total * FF ** (-0.5)).astype(jnp.bfloat16)


def whole_kernel(
    gate_hbm,
    up_hbm,
    down_hbm,
    gain_hbm,
    prompt_hbm,
    group_hbm,
    inner_hbm,
    weight_hbm,
    turn_hbm,
    gate_out,
    up_out,
    down_out,
    o_ref,
    held,
    gain,
    prompt,
    group,
    inner,
    weight,
    turn,
    s_ref,
    abuf,
    bbuf,
    f_ref,
    normed,
    served,
    part,
    xbuf,
    qbuf,
    nbuf,
    ubuf,
    rbuf,
    tbuf,
    load,
    store,
    send,
    recv,
):
    z = lax.axis_index("fs") // 2
    pairs = (
        (gain_hbm, gain),
        (gate_hbm, held.at[0]),
        (up_hbm, held.at[1]),
        (down_hbm, held.at[2]),
        (prompt_hbm, prompt),
        (turn_hbm, turn),
        (group_hbm, group),
        (inner_hbm, inner),
        (weight_hbm, weight),
    )
    loads = [pltpu.make_async_copy(a, b, load.at[n]) for n, (a, b) in enumerate(pairs)]
    stores = [
        pltpu.make_async_copy(served.at[n], out, store.at[n])
        for n, out in enumerate((gate_out, up_out, down_out))
    ]

    def ready():
        for copy in loads:
            copy.start()
        pack(gain, held, s_ref, loads[0], loads[1:4])

    def meanwhile():
        for copy in loads[4:]:
            copy.wait()
        values = prompt[...].astype(jnp.float32)
        normed[...] = (
            values * lax.rsqrt(jnp.mean(values * values, axis=1, keepdims=True) + 1e-06)
        ).astype(jnp.bfloat16)

    greet(partners(), ready)
    cp = Copies(send, recv)
    move(
        cp, s_ref, abuf, bbuf, f_ref, lambda w: settle_wave(w, z, f_ref, turn, served), meanwhile
    )
    for copy in stores:
        copy.start()
    partial_sums(z, normed, served, group, inner, weight, part)
    sum_parts(cp, part, o_ref, xbuf, qbuf, nbuf, ubuf, rbuf, tbuf)
    for copy in stores:
        copy.wait()
    cp.drain()
    assert cp.used <= SEMS, cp.used


def put_kernel(*refs):
    sources, targets, held, load, store = refs[:4], refs[4:8], refs[8:12], refs[12], refs[13]
    moves = []
    for i, pieces in ((3, 1), (0, PIECES), (1, PIECES), (2, PIECES)):
        size = sources[i].shape[0] // pieces
        for n in range(pieces):
            rows, at = pl.ds(n * size, size), len(moves)
            moves.append(
                (
                    pltpu.make_async_copy(sources[i].at[rows], held[i].at[rows], load.at[at]),
                    pltpu.make_async_copy(held[i].at[rows], targets[i].at[rows], store.at[at]),
                )
            )
    for get, _ in moves:
        get.start()
    for get, give in moves:
        get.wait()
        give.start()
    for _, give in moves:
        give.wait()


PIECES = 4


def put(*values):
    hbm = pl.BlockSpec(memory_space=pl.ANY)
    return pl.pallas_call(
        put_kernel,
        out_shape=tuple(jax.ShapeDtypeStruct(v.shape, v.dtype) for v in values),
        in_specs=[hbm] * 4,
        out_specs=(hbm,) * 4,
        scratch_shapes=[pltpu.VMEM(v.shape, v.dtype) for v in values]
        + [pltpu.SemaphoreType.DMA((3 * PIECES + 1,))] * 2,
        compiler_params=pltpu.CompilerParams(vmem_limit_bytes=58 << 20),
    )(*values)


def whole(gate, up, down, gain, prompt, group, inner, weight):
    hbm = pl.BlockSpec(memory_space=pl.ANY)
    out = jax.ShapeDtypeStruct((2048, 256), jnp.bfloat16)
    bf16, f32 = jnp.bfloat16, jnp.float32
    return pl.pallas_call(
        whole_kernel,
        out_shape=(out, out, out, jax.ShapeDtypeStruct((32, 256), bf16)),
        in_specs=[hbm] * 9,
        out_specs=(hbm, hbm, hbm, pl.BlockSpec(memory_space=pltpu.VMEM)),
        scratch_shapes=[
            pltpu.VMEM((3, 32, 32, 32), f32),
            pltpu.VMEM((1, 32), f32),
            pltpu.VMEM((256, 2048), bf16),
            pltpu.VMEM((1, 256), jnp.int32),
            pltpu.VMEM((2, 256), jnp.int32),
            pltpu.VMEM((2, 256), f32),
            pltpu.VMEM((512, 512), bf16),
            pltpu.VMEM((4, 8, 24, 128), bf16),
            pltpu.VMEM((4, 8, 24, 128), bf16),
            pltpu.VMEM((2, 3, 3, 4, 24, 128), bf16),
            pltpu.VMEM((2, 4, 64, 24, 128), bf16),
            pltpu.VMEM((256, 2048), bf16),
            pltpu.VMEM((3, 2048, 256), bf16),
            pltpu.VMEM((2, 4, 8, 32, 256), bf16),
            pltpu.VMEM((4, 8, 32, 256), bf16),
            pltpu.VMEM((4, 8, 32, 256), bf16),
            pltpu.VMEM((3, 8, 32, 256), bf16),
            pltpu.VMEM((32, 256), bf16),
            pltpu.VMEM((2, 4, 32, 256), bf16),
            pltpu.VMEM((2, 3, 32, 256), bf16),
            pltpu.SemaphoreType.DMA((9,)),
            pltpu.SemaphoreType.DMA((3,)),
            pltpu.SemaphoreType.DMA((SEMS,)),
            pltpu.SemaphoreType.DMA((SEMS,)),
        ],
        compiler_params=pltpu.CompilerParams(
            collective_id=0, has_side_effects=True, vmem_limit_bytes=58 << 20
        ),
    )(gate, up, down, gain, prompt, group, inner, weight, jnp.asarray(turning(), bf16))


def shards(
    prompt, norm_gain, gate_master, up_master, down_master, group_choice, inner_choice, route_weight
):
    gate, up, down, mixed = whole(
        gate_master,
        up_master,
        down_master,
        norm_gain[None, :],
        prompt,
        group_choice[None, :],
        inner_choice.T,
        route_weight.T,
    )
    gate, up, down, mixed = put(gate, up, down, mixed)
    return gate, up, down, mixed.T


def solution(mesh):
    in_specs = (
        P("tp", None),
        P("fs"),
        P(None, "fs", "tp"),
        P(None, "fs", "tp"),
        P(None, "fs", "tp"),
        P("tp"),
        P("tp", None),
        P("tp", None),
    )
    out_specs = (P(None, "fs"), P(None, "fs"), P(None, "fs"), P("tp", "fs"))
    return jax.shard_map(
        shards, mesh=mesh, in_specs=in_specs, out_specs=out_specs, check_vma=False
    )
```
